32 devices in a mesh: grp: 2 (over y), fs: 4 (over z), tp: 4 (over x, core).
Axes of the slice: x: 2, y: 2, z: 4, core: 2. Of those that a mesh axis runs over, the one named last changes fastest.
Arguments:
- tokens: bfloat16 [2048, 2048], P(('grp', 'fs'), 'tp'), parts along dimension 0, may hold values from -6 to 6
- recurrent_norm_gain: float32 [2048], replicated, may hold values from 0.1 to 1.9
- feedforward_norm_gain: float32 [2048], replicated, may hold values from 0.1 to 1.9
- gate_projection_weight: bfloat16 [2048, 2048], P('fs', 'tp'), may hold values from -0.125 to 0.125
- recurrent_projection_weight: bfloat16 [2048, 2048], P('fs', 'tp'), may hold values from -0.125 to 0.125
- convolution_kernel: bfloat16 [4, 2048], P(None, 'tp'), may hold values from -3 to 3
- decay_gate_matrix: bfloat16 [16, 128, 128], P('tp'), may hold values from -0.5 to 0.5
- input_gate_matrix: bfloat16 [16, 128, 128], P('tp'), may hold values from -0.5 to 0.5
- base_decay_logit: float32 [2048], P('tp'), may hold values from 3 to 9
- extra_log_decay: float32 [2048], P(('grp', 'fs')), parts along dimension 0, may hold values from -0.7 to 0
- output_projection_weight: bfloat16 [2048, 2048], P('tp', 'fs'), may hold values from -0.125 to 0.125
- up_projection_weight: bfloat16 [2048, 8192], P('fs', 'tp'), may hold values from -0.125 to 0.125
- down_projection_weight: bfloat16 [8192, 2048], P('tp', 'fs'), may hold values from -0.0625 to 0.0625
Outputs:
- layer_out: bfloat16 [2048, 2048], P(('grp', 'fs'), 'tp'), parts along dimension 0
The draws below stay inside these ranges and needn't reach their ends.
There are 2 independent parts, one for each index of `grp`. The reference program is written for one: setup_inputs(seed, part) draws one part's arguments, and reference() takes and returns one part's arrays. A program takes and returns all parts, laid end to end along the dimension named above; an argument that names none is the same for every part. Nothing has to cross between parts.
All inputs are finite; a program needn't handle non-finite values.
Results may differ from the reference program's by a relative error of at most 0.018.
Values may be sent and summed in bfloat16 or wider, within the bound.
No kernel may reach another device: no remote copies, remote signals or barrier semaphores. Data moves between devices by JAX's collectives and lax.ppermute only.
A program may use at most 64 MiB of HBM per device.

```python
import math
import jax
import jax.numpy as jnp
from jax import lax

D = 2048
FF = 8192
BLOCKS = 16
BLOCK_DIM = 128
CONV = 4
SEQUENCE_TOKENS = 256
WIDTH = 2048
TOKENS = 1024
N_TP = 4


def draw_base_decay_logit(key, part):
    key_pick, key_slow, key_fast = jax.random.split(key, 3)
    share = 0.5
    chosen = jax.random.uniform(key_pick, (WIDTH,), jnp.float32) < share
    slow_rate = jnp.exp(jax.random.uniform(key_slow, (WIDTH,), jnp.float32, math.log(0.3), math.log(1.5))) / (4.0 * SEQUENCE_TOKENS)
    fast_rate = 0.25 / jnp.exp(jax.random.uniform(key_fast, (WIDTH,), jnp.float32, math.log(8.0), math.log(25.0)))
    decay_rate = jnp.where(chosen, fast_rate, slow_rate)
    return (-decay_rate - jnp.log(-jnp.expm1(-decay_rate))).astype(jnp.float32)


def draw_extra_log_decay(key, part):
    key_pick, key_depth = jax.random.split(key)
    picked = jax.random.randint(key_pick, (TOKENS,), 0, SEQUENCE_TOKENS) < 3
    depth = jnp.log(jax.random.uniform(key_depth, (TOKENS,), jnp.float32, 0.5, 0.8))
    return jnp.where(picked, depth, 0.0).astype(jnp.float32)


def block_levels(stream_key, shape, cuts, low, largest):
    gain, own = 1.0, jax.random.fold_in(stream_key, 6)
    for axis_at, shards_of in cuts:
        steps = jnp.exp(jax.random.uniform(jax.random.fold_in(own, axis_at), (shards_of,), jnp.float32, low / len(cuts), largest / len(cuts)))
        gain = gain * jnp.repeat(steps, shape[axis_at] // shards_of).reshape([-1 if axis == axis_at else 1 for axis in range(len(shape))])
    return gain


def noise(rng, shape, spread, bound, pieces=(), dtype=jnp.bfloat16):
    drawn = spread * jax.random.normal(rng, shape, jnp.float32)
    if pieces:
        drawn = drawn * block_levels(rng, shape, pieces, -0.22, 0.18)
    return jnp.clip(drawn, -bound, bound).astype(dtype)


def setup_inputs(seed: int = 0, part: int = 0) -> dict:
    key_list = jax.random.split(jax.random.key(seed), 14)
    part_keys = jax.random.split(jax.random.fold_in(key_list[13], part), 14)
    tokens = noise(part_keys[0], (TOKENS, D), 1.0, 6.0, ((0, 4), (1, 4)))
    recurrent_norm_gain = jnp.clip(1.0 + 0.18 * jax.random.normal(key_list[1], (D,), jnp.float32), 0.1, 1.9)
    feedforward_norm_gain = jnp.clip(1.0 + 0.18 * jax.random.normal(key_list[2], (D,), jnp.float32), 0.1, 1.9)
    gate_projection_weight = noise(key_list[3], (D, WIDTH), D ** -0.5, 0.125, ((0, 4), (1, 4)))
    recurrent_projection_weight = noise(key_list[4], (D, WIDTH), D ** -0.5, 0.125, ((0, 4), (1, 4)))
    convolution_kernel = noise(key_list[5], (CONV, WIDTH), 0.5, 3.0, ((1, 4),))
    decay_gate_matrix = noise(key_list[6], (BLOCKS, BLOCK_DIM, BLOCK_DIM), BLOCK_DIM ** -0.5, 0.5, ((0, 4),))
    input_gate_matrix = noise(key_list[7], (BLOCKS, BLOCK_DIM, BLOCK_DIM), BLOCK_DIM ** -0.5, 0.5, ((0, 4),))
    base_decay_logit = draw_base_decay_logit(jax.random.fold_in(key_list[13], 71), part)
    extra_log_decay = draw_extra_log_decay(jax.random.fold_in(jax.random.fold_in(key_list[13], part), 71), part)
    output_projection_weight = noise(key_list[10], (WIDTH, D), WIDTH ** -0.5, 0.125, ((0, 4), (1, 4)))
    up_projection_weight = noise(key_list[11], (D, FF), D ** -0.5, 0.125, ((0, 4), (1, 4)))
    down_projection_weight = noise(key_list[12], (FF, D), FF ** -0.5, 0.0625, ((0, 4), (1, 4)))
    return dict(tokens=tokens, recurrent_norm_gain=recurrent_norm_gain, feedforward_norm_gain=feedforward_norm_gain, gate_projection_weight=gate_projection_weight, recurrent_projection_weight=recurrent_projection_weight, convolution_kernel=convolution_kernel, decay_gate_matrix=decay_gate_matrix, input_gate_matrix=input_gate_matrix, base_decay_logit=base_decay_logit, extra_log_decay=extra_log_decay, output_projection_weight=output_projection_weight, up_projection_weight=up_projection_weight, down_projection_weight=down_projection_weight)


def rms_rows(values_in, norm_gain):
    values = values_in.astype(jnp.float32)
    inverse = lax.rsqrt(lax.optimization_barrier(jnp.mean(values * values, axis=-1, keepdims=True)) + 1e-06)
    return (values * inverse * norm_gain.astype(jnp.float32)).astype(jnp.bfloat16)

def combine(earlier, later):
    return (earlier[0] * later[0], later[0] * earlier[1] + later[1])

def recurrent_state(recurrent_branch_rows, gate_branch_rows, convolution_kernel, decay_gate_matrix, input_gate_matrix, base_decay_logit, extra_log_decay):
    length = recurrent_branch_rows.shape[0]
    taps = convolution_kernel.shape[0]
    padded = jnp.pad(recurrent_branch_rows.astype(jnp.float32), ((taps - 1, 0), (0, 0)))
    conv_sum = jnp.zeros((length, recurrent_branch_rows.shape[1]), jnp.float32)
    for tap_index in range(taps):
        conv_sum = conv_sum + padded[tap_index:tap_index + length] * convolution_kernel[tap_index].astype(jnp.float32)
    conv_rows = conv_sum.astype(jnp.bfloat16)
    blocks = decay_gate_matrix.shape[0]
    blocked = conv_rows.reshape(length, blocks, -1).astype(jnp.float32)
    recurrence_gate = jax.nn.sigmoid(jnp.einsum('tni,nij->tnj', blocked, decay_gate_matrix.astype(jnp.float32)).reshape(length, -1))
    input_rate = jax.nn.sigmoid(jnp.einsum('tni,nij->tnj', blocked, input_gate_matrix.astype(jnp.float32)).reshape(length, -1))
    decay_log_values = -8.0 * jax.nn.softplus(-base_decay_logit) * recurrence_gate + extra_log_decay[:, None]
    decay = jnp.exp(decay_log_values)
    drive = jnp.sqrt(-jnp.expm1(2.0 * decay_log_values)) * input_rate * conv_rows.astype(jnp.float32)
    _, hidden = lax.associative_scan(combine, (decay, drive), axis=0)
    return (hidden * gate_branch_rows.astype(jnp.float32)).astype(jnp.bfloat16)

def split_sum(left_rows, weight):
    block_width = weight.shape[0] // N_TP
    summed = jnp.zeros((left_rows.shape[0], weight.shape[1]), jnp.float32)
    for block_index in range(N_TP):
        lower = block_index * block_width
        partial_value = jnp.dot(left_rows[:, lower:lower + block_width], weight[lower:lower + block_width], preferred_element_type=jnp.float32).astype(jnp.bfloat16)
        summed = summed + lax.optimization_barrier(partial_value).astype(jnp.float32)
    return summed

def reference(tokens, recurrent_norm_gain, feedforward_norm_gain, gate_projection_weight, recurrent_projection_weight, convolution_kernel, decay_gate_matrix, input_gate_matrix, base_decay_logit, extra_log_decay, output_projection_weight, up_projection_weight, down_projection_weight):
    sequence_count = tokens.shape[0]
    sequence_batch = sequence_count // SEQUENCE_TOKENS
    normed = rms_rows(tokens, recurrent_norm_gain)
    gate_branch_rows = jax.nn.gelu(jnp.dot(normed, gate_projection_weight, preferred_element_type=jnp.float32)).astype(jnp.bfloat16)
    recurrent_branch_rows = jnp.dot(normed, recurrent_projection_weight, preferred_element_type=jnp.float32).astype(jnp.bfloat16)
    mixed_output = jax.vmap(recurrent_state, in_axes=(0, 0, None, None, None, None, 0))(recurrent_branch_rows.reshape(sequence_batch, SEQUENCE_TOKENS, -1), gate_branch_rows.reshape(sequence_batch, SEQUENCE_TOKENS, -1), convolution_kernel, decay_gate_matrix, input_gate_matrix, base_decay_logit, extra_log_decay.reshape(sequence_batch, SEQUENCE_TOKENS)).reshape(sequence_count, -1)
    residual = (tokens.astype(jnp.float32) + split_sum(mixed_output, output_projection_weight)).astype(jnp.bfloat16)
    channel_in = rms_rows(residual, feedforward_norm_gain)
    upward = jnp.maximum(jnp.dot(channel_in, up_projection_weight, preferred_element_type=jnp.float32), 0.0)
    squared = (upward * upward).astype(jnp.bfloat16)
    return (residual.astype(jnp.float32) + split_sum(squared, down_projection_weight)).astype(jnp.bfloat16)
```

```python
import jax
import jax.numpy as jnp
from jax import lax
from jax.sharding import PartitionSpec as P


def rms_rows(values_in, norm_gain):
    values = values_in.astype(jnp.float32)
    inverse = lax.rsqrt(jnp.mean(values * values, axis=-1, keepdims=True) + 1e-06)
    return (values * inverse * norm_gain).astype(jnp.bfloat16)


def combine(earlier, later):
    return (earlier[0] * later[0], later[0] * earlier[1] + later[1])


def recurrent_state(
    recurrent_branch_rows,
    gate_branch_rows,
    convolution_kernel,
    decay_gate_matrix,
    input_gate_matrix,
    base_decay_logit,
    extra_log_decay,
):
    length = recurrent_branch_rows.shape[0]
    taps = convolution_kernel.shape[0]
    padded = jnp.pad(recurrent_branch_rows.astype(jnp.float32), ((taps - 1, 0), (0, 0)))
    conv_sum = jnp.zeros((length, recurrent_branch_rows.shape[1]), jnp.float32)
    for tap_index in range(taps):
        conv_sum = conv_sum + padded[tap_index : tap_index + length] * convolution_kernel[
            tap_index
        ].astype(jnp.float32)
    conv_rows = conv_sum.astype(jnp.bfloat16)
    blocks = decay_gate_matrix.shape[0]
    blocked = conv_rows.reshape(length, blocks, -1)
    recurrence_gate = jax.nn.sigmoid(
        jnp.einsum(
            "tni,nij->tnj", blocked, decay_gate_matrix, preferred_element_type=jnp.float32
        ).reshape(length, -1)
    )
    input_rate = jax.nn.sigmoid(
        jnp.einsum(
            "tni,nij->tnj", blocked, input_gate_matrix, preferred_element_type=jnp.float32
        ).reshape(length, -1)
    )
    decay_log_values = (
        -8.0 * jax.nn.softplus(-base_decay_logit) * recurrence_gate + extra_log_decay[:, None]
    )
    decay = jnp.exp(decay_log_values)
    drive = (
        jnp.sqrt(-jnp.expm1(2.0 * decay_log_values)) * input_rate * conv_rows.astype(jnp.float32)
    )
    _, hidden = lax.associative_scan(combine, (decay, drive), axis=0)
    return (hidden * gate_branch_rows.astype(jnp.float32)).astype(jnp.bfloat16)


def per_device_plain(
    tokens,
    recurrent_norm_gain,
    feedforward_norm_gain,
    gate_projection_weight,
    recurrent_projection_weight,
    convolution_kernel,
    decay_gate_matrix,
    input_gate_matrix,
    base_decay_logit,
    extra_log_decay,
    output_projection_weight,
    up_projection_weight,
    down_projection_weight,
):
    whole_rows = lax.all_gather(tokens, "tp", axis=1, tiled=True)
    normed = rms_rows(whole_rows, recurrent_norm_gain)
    columns = normed
    gate_pre = jnp.dot(
        columns,
        lax.all_gather(gate_projection_weight, "fs", axis=0, tiled=True),
        preferred_element_type=jnp.float32,
    )
    recur_pre = jnp.dot(
        columns,
        lax.all_gather(recurrent_projection_weight, "fs", axis=0, tiled=True),
        preferred_element_type=jnp.float32,
    )
    gate_branch_rows = jax.nn.gelu(gate_pre).astype(jnp.bfloat16)
    recurrent_branch_rows = recur_pre.astype(jnp.bfloat16)
    mixed_output = recurrent_state(
        recurrent_branch_rows,
        gate_branch_rows,
        convolution_kernel,
        decay_gate_matrix,
        input_gate_matrix,
        base_decay_logit,
        extra_log_decay,
    )
    partials = jnp.dot(
        mixed_output,
        lax.all_gather(output_projection_weight, "fs", axis=1, tiled=True),
        preferred_element_type=jnp.float32,
    )
    residual = (
        tokens.astype(jnp.float32)
        + lax.psum_scatter(
            partials.astype(jnp.bfloat16), "tp", scatter_dimension=1, tiled=True
        ).astype(jnp.float32)
    ).astype(jnp.bfloat16)
    middle = lax.all_gather(residual, "tp", axis=1, tiled=True)
    channel_in = rms_rows(middle, feedforward_norm_gain)
    columns = channel_in
    upward = jnp.dot(
        columns,
        lax.all_gather(up_projection_weight, "fs", axis=0, tiled=True),
        preferred_element_type=jnp.float32,
    )
    positive = jnp.maximum(upward, 0.0)
    squared = (positive * positive).astype(jnp.bfloat16)
    down_terms = jnp.dot(
        squared,
        lax.all_gather(down_projection_weight, "fs", axis=1, tiled=True),
        preferred_element_type=jnp.float32,
    )
    summed_down = lax.psum_scatter(
        down_terms.astype(jnp.bfloat16), "tp", scatter_dimension=1, tiled=True
    ).astype(jnp.float32)
    return (residual.astype(jnp.float32) + summed_down).astype(jnp.bfloat16)


def shift_pairs(size):
    return [(i, (i + 1) % size) for i in range(size)]


def gather_features(block):
    n = lax.axis_size("tp")
    me = lax.axis_index("tp")
    same_core = [block]
    for j in range(2, n, 2):
        same_core.append(lax.ppermute(block, "tp", [(i, i ^ j) for i in range(n)]))
    swap = [(i, i ^ 1) for i in range(n)]
    pieces = []
    for piece in same_core:
        pieces.append(piece)
        pieces.append(lax.ppermute(piece, "tp", swap))
    stacked = jnp.stack(pieces)
    ordered = [lax.dynamic_index_in_dim(stacked, me ^ p, 0, False) for p in range(n)]
    return jnp.concatenate(ordered, axis=1)


def scatter_features(partials):
    n = lax.axis_size("tp")
    me = lax.axis_index("tp")
    width = partials.shape[1] // n

    def block(owner):
        return lax.dynamic_slice_in_dim(partials, owner * width, width, 1)

    total = block(me).astype(jnp.float32)
    for j in range(n - 1, 0, -1):
        arrived = lax.ppermute(block(me ^ j), "tp", [(i, i ^ j) for i in range(n)])
        total = total + arrived.astype(jnp.float32)
    return total


def dot32(a, b):
    return jnp.dot(a, b, preferred_element_type=jnp.float32)


def per_device(
    tokens,
    recurrent_norm_gain,
    feedforward_norm_gain,
    gate_projection_weight,
    recurrent_projection_weight,
    convolution_kernel,
    decay_gate_matrix,
    input_gate_matrix,
    base_decay_logit,
    extra_log_decay,
    output_projection_weight,
    up_projection_weight,
    down_projection_weight,
):
    fs = lax.axis_size("fs")
    f = lax.axis_index("fs")
    g = lax.axis_index("grp")
    first = g == 0
    around = shift_pairs(fs)
    across = [(0, 1), (1, 0)]

    gate_w, recur_w = gate_projection_weight, recurrent_projection_weight
    gr = [jnp.where(first, gate_w, recur_w), jnp.where(first, recur_w, gate_w)]
    out_rows = output_projection_weight.shape[0] // 2
    out = [
        lax.dynamic_slice_in_dim(output_projection_weight, h * out_rows, out_rows, 0)
        for h in (g, 1 - g)
    ]
    quarter = up_projection_weight.shape[1] // 4
    starts = [(2 * g + c) * quarter for c in range(2)] + [(2 * (1 - g) + c) * quarter for c in range(2)]
    up = [lax.dynamic_slice_in_dim(up_projection_weight, at, quarter, 1) for at in starts]
    down = [lax.dynamic_slice_in_dim(down_projection_weight, at, quarter, 0) for at in starts]

    streams = {"gr": gr[0], "out": out[0], "upa": up[0], "upb": up[1], "dna": down[0], "dnb": down[1]}
    mine = {name: [] for name in streams}
    other = {name: [] for name in streams}
    for name, block in streams.items():
        held = block
        for k in range(1, fs):
            with jax.named_scope(f"z_{name}_{k}"):
                held = lax.ppermute(held, "fs", around)
            mine[name].append(held)
            with jax.named_scope(f"y_{name}_{k}"):
                other[name].append(lax.ppermute(held, "grp", across))
    mine["gr"].insert(0, gr[0])
    other["gr"].insert(0, gr[1])
    mine["out"].insert(0, out[0])
    other["out"].insert(0, out[1])
    for at, name in enumerate(("upa", "upb")):
        mine[name].insert(0, up[at])
        other[name].insert(0, up[at + 2])
    for at, name in enumerate(("dna", "dnb")):
        mine[name].insert(0, down[at])
        other[name].insert(0, down[at + 2])

    def sources(rows_in):
        width = rows_in.shape[1] // fs
        return [
            lax.dynamic_slice_in_dim(rows_in, ((f - k + fs) % fs) * width, width, 1)
            for k in range(fs)
        ]

    def summed(left, blocks):
        total = dot32(left[0], blocks[0])
        for a, b in zip(left[1:], blocks[1:]):
            total = total + dot32(a, b)
        return total

    def in_order(parts):
        stacked = jnp.stack(parts)
        return jnp.concatenate(
            [lax.dynamic_index_in_dim(stacked, (f - p + fs) % fs, 0, False) for p in range(fs)],
            axis=1,
        )

    normed = rms_rows(gather_features(tokens), recurrent_norm_gain)
    left = sources(normed)
    pre = [summed(left, mine["gr"]), summed(left, other["gr"])]
    gate_branch_rows = jax.nn.gelu(jnp.where(first, pre[0], pre[1])).astype(jnp.bfloat16)
    recurrent_branch_rows = jnp.where(first, pre[1], pre[0]).astype(jnp.bfloat16)
    mixed = recurrent_state(
        recurrent_branch_rows,
        gate_branch_rows,
        convolution_kernel,
        decay_gate_matrix,
        input_gate_matrix,
        base_decay_logit,
        extra_log_decay,
    )
    halves = [lax.dynamic_slice_in_dim(mixed, h * out_rows, out_rows, 1) for h in (g, 1 - g)]
    partials = in_order(
        [
            (dot32(halves[0], a) + dot32(halves[1], b)).astype(jnp.bfloat16)
            for a, b in zip(mine["out"], other["out"])
        ]
    )
    residual = (tokens.astype(jnp.float32) + scatter_features(partials)).astype(jnp.bfloat16)
    channel_in = rms_rows(gather_features(residual), feedforward_norm_gain)
    left = sources(channel_in)
    squared = []
    for blocks in (mine["upa"], mine["upb"], other["upa"], other["upb"]):
        positive = jnp.maximum(summed(left, blocks), 0.0)
        squared.append((positive * positive).astype(jnp.bfloat16))
    down_terms = in_order(
        [
            summed(squared, blocks).astype(jnp.bfloat16)
            for blocks in zip(mine["dna"], mine["dnb"], other["dna"], other["dnb"])
        ]
    )
    return (residual.astype(jnp.float32) + scatter_features(down_terms)).astype(jnp.bfloat16)


def solution(mesh):
    placed = (
        P(("grp", "fs"), "tp"),
        P(),
        P(),
        P("fs", "tp"),
        P("fs", "tp"),
        P(None, "tp"),
        P("tp", None, None),
        P("tp", None, None),
        P("tp"),
        P(("grp", "fs")),
        P("tp", "fs"),
        P("fs", "tp"),
        P("tp", "fs"),
    )
    return jax.shard_map(
        per_device, mesh=mesh, in_specs=placed, out_specs=P(("grp", "fs"), "tp"), check_vma=False
    )
```

```python
import jax
import jax.numpy as jnp
from jax import lax
from jax.experimental import pallas as pl
from jax.experimental.pallas import tpu as pltpu
from jax.sharding import PartitionSpec as P


VMEM_SPEC = pl.BlockSpec(memory_space=pltpu.VMEM)
SMEM_SPEC = pl.BlockSpec(memory_space=pltpu.SMEM)


def cost(flops, *arrays):
    size = sum(a.size * a.dtype.itemsize for a in arrays)
    return pl.CostEstimate(flops=int(flops), bytes_accessed=int(size), transcendentals=0)


def norm_kernel(me_ref, gain_ref, *refs):
    *pieces, normed_ref = refs
    me = me_ref[0]
    width = pieces[0].shape[1]
    total = jnp.zeros((pieces[0].shape[0], 1), jnp.float32)
    for piece in pieces:
        values = piece[...].astype(jnp.float32)
        total = total + jnp.sum(values * values, axis=-1, keepdims=True)
    inverse = lax.rsqrt(total / (width * len(pieces)) + 1e-06)
    for j, piece in enumerate(pieces):
        columns = pl.ds(pl.multiple_of((me ^ j) * width, width), width)
        values = piece[...].astype(jnp.float32)
        normed_ref[:, columns] = (values * inverse * gain_ref[:, columns]).astype(jnp.bfloat16)


def norm_pieces(pieces, norm_gain):
    rows, width = pieces[0].shape
    features = width * len(pieces)
    return pl.pallas_call(
        norm_kernel,
        out_shape=jax.ShapeDtypeStruct((rows, features), jnp.bfloat16),
        in_specs=[SMEM_SPEC] + [VMEM_SPEC] * (1 + len(pieces)),
        out_specs=VMEM_SPEC,
        cost_estimate=cost(60e6, *pieces, *pieces),
        name="norm_pieces",
    )(lax.axis_index("tp").reshape(1), norm_gain.reshape(1, features), *pieces)


def one_minus_exp(x):
    series = jnp.full_like(x, 1.0 / 5040)
    for coefficient in (1.0 / 720, 1.0 / 120, 1.0 / 24, 1.0 / 6, 0.5, 1.0):
        series = series * x + coefficient
    return jnp.where(x > -0.3, -x * series, 1.0 - jnp.exp(x))


def recurrent_kernel(
    first_ref,
    pre_a_ref,
    pre_b_ref,
    taps_ref,
    decay_matrix_ref,
    input_matrix_ref,
    rate_ref,
    extra_ref,
    mixed_ref,
    decay_ref,
    drive_ref,
):
    first = first_ref[0] == 1
    rows, width = pre_a_ref.shape
    blocks, block, _ = decay_matrix_ref.shape
    taps = taps_ref.shape[0]
    row = lax.broadcasted_iota(jnp.int32, (rows, block), 0)
    within = row % 8
    for n in range(blocks):
        at = slice(n * block, (n + 1) * block)
        recur = jnp.where(first, pre_b_ref[:, at], pre_a_ref[:, at])
        recur = recur.astype(jnp.bfloat16).astype(jnp.float32)
        conv = jnp.zeros((rows, block), jnp.float32)
        for tap in range(taps):
            back = taps - 1 - tap
            moved = recur if back == 0 else jnp.where(row >= back, pltpu.roll(recur, back, 0), 0.0)
            conv = conv + moved * taps_ref[tap : tap + 1, at].astype(jnp.float32)
        conv_rows = conv.astype(jnp.bfloat16)
        recur_gate = jax.nn.sigmoid(dot32(conv_rows, decay_matrix_ref[n]))
        input_rate = jax.nn.sigmoid(dot32(conv_rows, input_matrix_ref[n]))
        log_decay = rate_ref[:, at] * recur_gate + extra_ref[...]
        decay = jnp.exp(log_decay)
        drive = jnp.sqrt(one_minus_exp(2.0 * log_decay)) * input_rate * conv_rows.astype(jnp.float32)
        for step in (1, 2, 4):
            inside = within >= step
            earlier_drive = jnp.where(inside, pltpu.roll(drive, step, 0), 0.0)
            earlier_decay = jnp.where(inside, pltpu.roll(decay, step, 0), 1.0)
            drive = drive + decay * earlier_drive
            decay = decay * earlier_decay
        decay_ref[:, at] = decay
        drive_ref[:, at] = drive
    carry = jnp.zeros((1, width), jnp.float32)
    for tile in range(rows // 8):
        at = slice(tile * 8, tile * 8 + 8)
        hidden = drive_ref[at] + decay_ref[at] * carry
        carry = hidden[7:8]
        gate = jax.nn.gelu(jnp.where(first, pre_a_ref[at], pre_b_ref[at]))
        gate = gate.astype(jnp.bfloat16).astype(jnp.float32)
        drive_ref[at] = hidden * gate
    mixed_ref[...] = drive_ref[...].astype(jnp.bfloat16)


def recurrent_rows(first, pre_a, pre_b, taps, decay_matrix, input_matrix, base_decay_logit, extra):
    rows, width = pre_a.shape
    rate = (-8.0 * jax.nn.softplus(-base_decay_logit)).reshape(1, width)
    return pl.pallas_call(
        recurrent_kernel,
        out_shape=jax.ShapeDtypeStruct((rows, width), jnp.bfloat16),
        in_specs=[SMEM_SPEC] + [VMEM_SPEC] * 7,
        out_specs=VMEM_SPEC,
        scratch_shapes=[pltpu.VMEM((rows, width), jnp.float32)] * 2,
        cost_estimate=cost(2e9, pre_a, pre_b),
        name="recurrent_rows",
    )(
        first.astype(jnp.int32).reshape(1),
        pre_a,
        pre_b,
        taps,
        decay_matrix,
        input_matrix,
        rate,
        extra.reshape(rows, 1),
    )


def shift_pairs(size, stride):
    return [(i, (i + stride) % size) for i in range(size)]


def gather_features(block):
    n = lax.axis_size("tp")
    same_core = [block]
    for j in range(2, n, 2):
        same_core.append(lax.ppermute(block, "tp", [(i, i ^ j) for i in range(n)]))
    swap = [(i, i ^ 1) for i in range(n)]
    pieces = []
    for piece in same_core:
        pieces.append(piece)
        pieces.append(lax.ppermute(piece, "tp", swap))
    return pieces


def scatter_features(partials):
    n = lax.axis_size("tp")
    me = lax.axis_index("tp")
    width = partials.shape[1] // n

    def block(owner):
        return lax.dynamic_slice_in_dim(partials, owner * width, width, 1)

    total = block(me).astype(jnp.float32)
    for j in range(n - 1, 0, -1):
        arrived = lax.ppermute(block(me ^ j), "tp", [(i, i ^ j) for i in range(n)])
        total = total + arrived.astype(jnp.float32)
    return total


def dot32(a, b):
    return jnp.dot(a, b, preferred_element_type=jnp.float32)


def layer(
    tokens,
    recurrent_norm_gain,
    feedforward_norm_gain,
    gate_projection_weight,
    recurrent_projection_weight,
    convolution_kernel,
    decay_gate_matrix,
    input_gate_matrix,
    base_decay_logit,
    extra_log_decay,
    output_projection_weight,
    up_projection_weight,
    down_projection_weight,
):
    fs = lax.axis_size("fs")
    f = lax.axis_index("fs")
    g = lax.axis_index("grp")
    first = g == 0
    pair = [(i, i ^ 1) for i in range(fs)]
    across = [(0, 1), (1, 0)]

    gate_w, recur_w = gate_projection_weight, recurrent_projection_weight
    gr = [jnp.where(first, gate_w, recur_w), jnp.where(first, recur_w, gate_w)]
    out_rows = output_projection_weight.shape[0] // 2
    out = [
        lax.dynamic_slice_in_dim(output_projection_weight, h * out_rows, out_rows, 0)
        for h in (g, 1 - g)
    ]
    quarter = up_projection_weight.shape[1] // 4
    starts = [(2 * g + c) * quarter for c in range(2)] + [(2 * (1 - g) + c) * quarter for c in range(2)]
    up = [lax.dynamic_slice_in_dim(up_projection_weight, at, quarter, 1) for at in starts]
    down = [lax.dynamic_slice_in_dim(down_projection_weight, at, quarter, 0) for at in starts]

    blocks_of = {"gr": gr, "out": out, "upa": up[0::2], "upb": up[1::2], "dna": down[0::2], "dnb": down[1::2]}
    rings = {name: (1, fs) for name in blocks_of}
    rings["upa"] = rings["upb"] = (2, fs // 2)
    mine, other = {}, {}
    for name, (block, rest) in blocks_of.items():
        stride, rounds = rings[name]
        mine[name], other[name] = [block], [rest]
        for _ in range(1, rounds):
            block = lax.ppermute(block, "fs", shift_pairs(fs, stride))
            mine[name].append(block)
            other[name].append(lax.ppermute(block, "grp", across))

    def sources(rows_in, stride):
        width = rows_in.shape[1] // fs
        return [
            lax.dynamic_slice_in_dim(rows_in, ((f - k + fs) % fs) * width, width, 1)
            for k in range(0, fs, stride)
        ]

    def summed(left, blocks):
        total = dot32(left[0], blocks[0])
        for a, b in zip(left[1:], blocks[1:]):
            total = total + dot32(a, b)
        return total

    def in_order(parts):
        stacked = jnp.stack(parts)
        return jnp.concatenate(
            [lax.dynamic_index_in_dim(stacked, (f - p + fs) % fs, 0, False) for p in range(fs)],
            axis=1,
        )

    normed = norm_pieces(gather_features(tokens), recurrent_norm_gain)
    left = sources(normed, 1)
    pre = [summed(left, mine["gr"]), summed(left, other["gr"])]
    mixed = recurrent_rows(
        first,
        pre[0],
        pre[1],
        convolution_kernel,
        decay_gate_matrix,
        input_gate_matrix,
        base_decay_logit,
        extra_log_decay,
    )
    halves = [lax.dynamic_slice_in_dim(mixed, h * out_rows, out_rows, 1) for h in (g, 1 - g)]
    partials = in_order(
        [
            (dot32(halves[0], a) + dot32(halves[1], b)).astype(jnp.bfloat16)
            for a, b in zip(mine["out"], other["out"])
        ]
    )
    residual = (tokens.astype(jnp.float32) + scatter_features(partials)).astype(jnp.bfloat16)
    partner_residual = lax.ppermute(residual, "fs", pair)
    both = [gather_features(partner_residual), gather_features(residual)]
    channel_in = jnp.concatenate([norm_pieces(pieces, feedforward_norm_gain) for pieces in both])
    left = sources(channel_in, 2)
    rows = residual.shape[0]
    squared = []
    for blocks in (mine["upa"], mine["upb"], other["upa"], other["upb"]):
        upward = summed(left, blocks)
        arrived = lax.ppermute(upward[:rows].astype(jnp.bfloat16), "fs", pair)
        positive = jnp.maximum(upward[rows:] + arrived.astype(jnp.float32), 0.0)
        squared.append((positive * positive).astype(jnp.bfloat16))
    down_terms = in_order(
        [
            summed(squared, blocks).astype(jnp.bfloat16)
            for blocks in zip(mine["dna"], mine["dnb"], other["dna"], other["dnb"])
        ]
    )
    return (residual.astype(jnp.float32) + scatter_features(down_terms)).astype(jnp.bfloat16)


def solution(mesh):
    placed = (
        P(("grp", "fs"), "tp"),
        P(),
        P(),
        P("fs", "tp"),
        P("fs", "tp"),
        P(None, "tp"),
        P("tp", None, None),
        P("tp", None, None),
        P("tp"),
        P(("grp", "fs")),
        P("tp", "fs"),
        P("fs", "tp"),
        P("tp", "fs"),
    )
    return jax.shard_map(
        layer, mesh=mesh, in_specs=placed, out_specs=P(("grp", "fs"), "tp"), check_vma=False
    )
```
